32 devices in a mesh: sp: 4 (over z), fs: 4 (over y, x), tp: 2 (over core).
Axes of the slice: x: 2, y: 2, z: 4, core: 2. Of those that a mesh axis runs over, the one named last changes fastest.
Arguments:
- tokens: bfloat16 [4, 1024, 2048], P('fs', 'sp', 'tp'), may hold values from -6 to 6
- norm_gain: float32 [2048], replicated, may hold values from 0.1 to 1.9
- memory_query: bfloat16 [2048, 1024], P('fs', 'tp'), may hold values from -0.125 to 0.125
- memory_key: bfloat16 [2048, 1024], P('fs', 'tp'), may hold values from -0.125 to 0.125
- memory_value: bfloat16 [2048, 1024], P('fs', 'tp'), may hold values from -0.125 to 0.125
- memory_outgate: bfloat16 [2048, 1024], P('fs', 'tp'), may hold values from -0.125 to 0.125
- memory_ingate: bfloat16 [2048, 4], P(None, 'tp'), may hold values from -0.125 to 0.125
- memory_forget: bfloat16 [2048, 4], P(None, 'tp'), may hold values from -0.125 to 0.125
- forget_bias: float32 [4], P('tp'), may hold values from 3 to 13
- forget_shift: float32 [4, 1024, 4], P('fs', 'sp', 'tp'), may hold values from -1.6 to 0
- stick_query: bfloat16 [2048, 512], P(None, 'tp'), may hold values from -0.125 to 0.125
- stick_key: bfloat16 [2048, 512], P(None, 'tp'), may hold values from -0.125 to 0.125
- stick_value: bfloat16 [2048, 512], P(None, 'tp'), may hold values from -0.125 to 0.125
- stick_bias: float32 [4], P('tp'), may hold values from -11 to -2
- memory_gain: float32 [1024], P('tp'), may hold values from 0.1 to 1.9
- stick_gain: float32 [512], P('tp'), may hold values from 0.1 to 1.9
- out_memory: bfloat16 [1024, 2048], P('tp'), may hold values from -0.15625 to 0.15625
- out_stick: bfloat16 [512, 2048], P('tp'), may hold values from -0.15625 to 0.15625
Outputs:
- mixed: bfloat16 [4, 1024, 2048], P('fs', ('sp', 'tp'))
The draws below stay inside these ranges and needn't reach their ends.
All inputs are finite; a program needn't handle non-finite values.
Results may differ from the reference program's by a relative error of at most 0.015.
Values may be sent and summed in bfloat16 or wider, within the bound.
A program may use at most 128 MiB of HBM per device.

```python
import jax
import jax.numpy as jnp
from jax import lax

D = 2048
HM = 4
DM = 256
HS = 4
DS = 128
TOK_DEV = 256
BLOCK = 128
SEQ = 1024
SEQS = 4
N_SP = 4


def draw_forget_bias(key, part):
    keys = jax.random.split(jax.random.fold_in(key, 11), 3)
    order = jax.random.permutation(keys[0], HM)
    fast_value = jax.random.uniform(keys[1], (HM,), jnp.float32, 3.0, 4.5)
    slow_value = jnp.log(jnp.float32(SEQ)) + jax.random.uniform(keys[2], (HM,), jnp.float32, 1.0, 2.0)
    return jnp.where(order < HM // 2, slow_value, fast_value)


def draw_forget_shift(key, part):
    keys = jax.random.split(jax.random.fold_in(key, 23), 3)
    spans = SEQ // TOK_DEV
    rate = jax.random.uniform(keys[0], (SEQS, spans, 1, HM), jnp.float32, 0.1, 1.0)
    constant_baseline = -jnp.broadcast_to(rate, (SEQS, spans, TOK_DEV, HM)).reshape(SEQS, SEQ, HM) / jnp.float32(SEQ)
    spots = jax.random.randint(keys[1], (SEQS, 3), 0, SEQ)
    layer_total = jnp.log(jax.random.uniform(keys[2], (SEQS, 3, HM), jnp.float32, 0.6, 0.8))
    pairing_tally = (jnp.arange(SEQ)[None, None, :] == spots[:, :, None]).astype(jnp.float32)
    segment_bundles = jnp.einsum('fwz,fwx->fzx', pairing_tally, layer_total)
    return constant_baseline + segment_bundles


def draw_stick_bias(key, part):
    keys = jax.random.split(jax.random.fold_in(key, 37), 3)
    order = jax.random.permutation(keys[0], HS)
    far_value = -jnp.log(jnp.float32(SEQ)) + jax.random.uniform(keys[1], (HS,), jnp.float32, -0.5, 0.5)
    near_value = jax.random.uniform(keys[2], (HS,), jnp.float32, -4.0, -2.0)
    return jnp.where(order < HS // 2, far_value, near_value)


def shard_levels(rng, dims, cuts, smallest, high):
    def one(axis_at, parts):
        draws = jax.random.uniform(jax.random.fold_in(jax.random.fold_in(rng, 6), axis_at), (parts,), jnp.float32, smallest / len(cuts), high / len(cuts))
        return jnp.repeat(jnp.exp(draws), dims[axis_at] // parts).reshape((-1,) + (1,) * (len(dims) - axis_at - 1))

    factor_of = one(*cuts[0])
    for cut in cuts[1:]:
        factor_of = factor_of * one(*cut)
    return factor_of


def centred(own_key, extent, scale, bound, pieces=(), kind=jnp.bfloat16):
    level = shard_levels(own_key, extent, pieces, -0.22, 0.18) if pieces else 1.0
    result = jax.random.normal(own_key, extent, jnp.float32) * scale * level
    return jnp.minimum(jnp.maximum(result, -bound), bound).astype(kind)


def setup_inputs(seed: int = 0) -> dict:
    key_list = jax.random.split(jax.random.key(seed), 19)
    return {
        "tokens": centred(key_list[0], (SEQS, SEQ, D), 1.0, 6.0, ((0, 4), (1, 4), (2, 2))),
        "norm_gain": jnp.clip(1.0 + 0.18 * jax.random.normal(key_list[1], (D,), jnp.float32), 0.1, 1.9),
        "memory_query": centred(key_list[2], (D, HM * DM), D ** -0.5, 0.125, ((0, 4), (1, 2))),
        "memory_key": centred(key_list[3], (D, HM * DM), D ** -0.5, 0.125, ((0, 4), (1, 2))),
        "memory_value": centred(key_list[4], (D, HM * DM), D ** -0.5, 0.125, ((0, 4), (1, 2))),
        "memory_outgate": centred(key_list[5], (D, HM * DM), D ** -0.5, 0.125, ((0, 4), (1, 2))),
        "memory_ingate": centred(key_list[6], (D, HM), D ** -0.5, 0.125, ((1, 2),)),
        "memory_forget": centred(key_list[7], (D, HM), D ** -0.5, 0.125, ((1, 2),)),
        "forget_bias": draw_forget_bias(jax.random.fold_in(key_list[18], 71), 0),
        "forget_shift": draw_forget_shift(jax.random.fold_in(key_list[18], 71), 0),
        "stick_query": centred(key_list[10], (D, HS * DS), D ** -0.5, 0.125, ((1, 2),)),
        "stick_key": centred(key_list[11], (D, HS * DS), D ** -0.5, 0.125, ((1, 2),)),
        "stick_value": centred(key_list[12], (D, HS * DS), D ** -0.5, 0.125, ((1, 2),)),
        "stick_bias": draw_stick_bias(jax.random.fold_in(key_list[18], 71), 0),
        "memory_gain": jnp.clip(1.0 + 0.18 * jax.random.normal(key_list[14], (HM * DM,), jnp.float32), 0.1, 1.9),
        "stick_gain": jnp.clip(1.0 + 0.18 * jax.random.normal(key_list[15], (HS * DS,), jnp.float32), 0.1, 1.9),
        "out_memory": centred(key_list[16], (HM * DM, D), (HM * DM + HS * DS) ** -0.5, 0.15625, ((0, 2),)),
        "out_stick": centred(key_list[17], (HS * DS, D), (HM * DM + HS * DS) ** -0.5, 0.15625, ((0, 2),)),
    }


epsilon = 1e-06
floor_neg = -1e+30
peak_value = lax.Precision.HIGHEST

def rounded(values):
    return lax.optimization_barrier(values.astype(jnp.bfloat16)).astype(jnp.float32)

def per_head_norm(values, gain):
    scale = lax.rsqrt(lax.optimization_barrier(jnp.mean(values * values, axis=-1, keepdims=True)) + epsilon)
    return values * scale * gain

def memory_block(state_carry, inputs):
    state_matrix, state_max = state_carry
    queries, key_rows, value_rows, log_forget, in_gate = inputs
    length = queries.shape[0]
    causal = jnp.tril(jnp.ones((length, length), dtype=bool))
    cumulative = jnp.cumsum(log_forget, axis=0)
    spread = cumulative[:, None, :] - cumulative[None, :, :] + in_gate[None, :, :]
    spread = jnp.where(causal[:, :, None], spread, floor_neg)
    carried_log = cumulative + state_max[None, :]
    running = jnp.maximum(carried_log, lax.optimization_barrier(jnp.max(spread, axis=1)))
    carried = jnp.exp(carried_log - running)
    scores = jnp.einsum('thd,shd->tsh', queries, key_rows, precision=peak_value) * jnp.exp(spread - running[:, None, :])
    numerator = carried[:, :, None] * jnp.einsum('thd,hde->the', queries, state_matrix, precision=peak_value)
    numerator = numerator + jnp.einsum('tsh,she->the', scores, value_rows, precision=peak_value)
    block_total = cumulative[-1]
    gap_logs = block_total[None, :] - cumulative + in_gate
    next_max = jnp.maximum(block_total + state_max, lax.optimization_barrier(jnp.max(gap_logs, axis=0)))
    decay_factor = jnp.exp(block_total + state_max - next_max)
    weights = jnp.exp(gap_logs - next_max[None, :])
    next_matrix = decay_factor[:, None, None] * state_matrix + jnp.einsum('sh,shd,she->hde', weights, key_rows, value_rows, precision=peak_value)
    return ((next_matrix, next_max), numerator)

def memory_mixer(queries, key_rows, value_rows, log_forget, in_gate):
    segment_list = SEQ // BLOCK

    def split_blocks(array):
        return array.reshape((segment_list, BLOCK) + array.shape[1:])
    initial = (jnp.zeros((HM, DM, DM), jnp.float32), jnp.full((HM,), floor_neg, jnp.float32))
    scaled = key_rows * DM ** (-0.5)
    _, outputs = lax.scan(memory_block, initial, (split_blocks(queries), split_blocks(scaled), split_blocks(value_rows), split_blocks(log_forget), split_blocks(in_gate)))
    return outputs.reshape(SEQ, HM, DM)

def stick_piece(queries, key_rows, value_rows, head_bias, query_pos, key_start):
    logits = jnp.einsum('thd,shd->hts', queries.astype(jnp.float32), key_rows.astype(jnp.float32), precision=peak_value)
    logits = logits * DS ** (-0.5) + head_bias[:, None, None]
    key_pos = key_start + jnp.arange(key_rows.shape[0], dtype=jnp.int32)
    visible = key_pos[None, :] < query_pos[:, None]
    keep_log = jnp.where(visible[None], jax.nn.log_sigmoid(-logits), jnp.float32(0.0))
    after = lax.cumsum(keep_log, axis=2, reverse=True) - keep_log
    weights = jnp.where(visible[None], jnp.exp(jax.nn.log_sigmoid(logits) + after), jnp.float32(0.0)).astype(jnp.bfloat16)
    partial_out = jnp.einsum('hts,shd->thd', weights.astype(jnp.float32), value_rows.astype(jnp.float32), precision=peak_value)
    return (partial_out, lax.optimization_barrier(jnp.sum(keep_log, axis=2)).T)

def stick_mixer(queries, key_rows, value_rows, head_bias):

    def span_out(span):
        first_row = span * TOK_DEV
        query_span = lax.dynamic_slice_in_dim(queries, first_row, TOK_DEV, 0)
        query_pos = first_row + jnp.arange(TOK_DEV, dtype=jnp.int32)

        def visit(offset, state_carry):
            accumulated, running_sum = state_carry
            key_start = ((span - offset) * TOK_DEV).astype(jnp.int32)
            keys_span = lax.dynamic_slice_in_dim(key_rows, key_start, TOK_DEV, 0)
            values_span = lax.dynamic_slice_in_dim(value_rows, key_start, TOK_DEV, 0)
            part_out, part_keep = stick_piece(query_span, keys_span, values_span, head_bias, query_pos, key_start)
            return (accumulated + jnp.exp(running_sum)[:, :, None] * part_out, running_sum + part_keep)
        initial = (jnp.zeros((TOK_DEV, HS, DS), jnp.float32), jnp.zeros((TOK_DEV, HS), jnp.float32))
        accumulated, _ = lax.fori_loop(0, span + 1, visit, initial)
        return accumulated
    outputs = lax.map(span_out, jnp.arange(N_SP, dtype=jnp.int32))
    return outputs.reshape(SEQ, HS, DS)

def reference(tokens, norm_gain, memory_query, memory_key, memory_value, memory_outgate, memory_ingate, memory_forget, forget_bias, forget_shift, stick_query, stick_key, stick_value, stick_bias, memory_gain, stick_gain, out_memory, out_stick):

    def one_sequence(inputs):
        rows_in, shift_rows = inputs
        values = rows_in.astype(jnp.float32)
        normed = (values * lax.rsqrt(lax.optimization_barrier(jnp.mean(values * values, axis=-1, keepdims=True)) + epsilon) * norm_gain).astype(jnp.bfloat16)

        def project(weight):
            return jnp.dot(normed, weight, preferred_element_type=jnp.float32)
        memory_shape = (SEQ, HM, DM)
        queries = rounded(project(memory_query)).reshape(memory_shape)
        key_rows = rounded(project(memory_key)).reshape(memory_shape)
        value_rows = rounded(project(memory_value)).reshape(memory_shape)
        out_gate = jax.nn.sigmoid(rounded(project(memory_outgate))).reshape(memory_shape)
        in_gate = project(memory_ingate)
        log_forget = jax.nn.log_sigmoid(project(memory_forget) + forget_bias) + shift_rows
        memory_out = memory_mixer(queries, key_rows, value_rows, log_forget, in_gate)
        mix_memory = per_head_norm(out_gate * memory_out, memory_gain.reshape(HM, DM)).reshape(SEQ, HM * DM).astype(jnp.bfloat16)
        stick_shape = (SEQ, HS, DS)
        stick_q = project(stick_query).astype(jnp.bfloat16).reshape(stick_shape)
        stick_k = project(stick_key).astype(jnp.bfloat16).reshape(stick_shape)
        stick_v = project(stick_value).astype(jnp.bfloat16).reshape(stick_shape)
        stick_out = stick_mixer(stick_q, stick_k, stick_v, stick_bias)
        mix_stick = per_head_norm(stick_out, stick_gain.reshape(HS, DS)).reshape(SEQ, HS * DS).astype(jnp.bfloat16)
        mixed = jnp.dot(mix_memory, out_memory, preferred_element_type=jnp.float32) + jnp.dot(mix_stick, out_stick, preferred_element_type=jnp.float32)
        return mixed.astype(jnp.bfloat16)
    return lax.map(one_sequence, (tokens, forget_shift))
```

```python
import functools

import jax
import jax.numpy as jnp
from jax import lax
from jax.experimental import pallas as pl
from jax.experimental.pallas import tpu as pltpu
from jax.sharding import PartitionSpec as P

MESH = pl.DeviceIdType.MESH
epsilon = 1e-06
floor_neg = -1e30
f32 = jnp.float32
bf16 = jnp.bfloat16

KEY, VALUE, QUERY, GATE = 0, 1, 2, 3


def dot(a, b, dims=((1,), (0,))):
    return lax.dot_general(a, b, (dims, ((), ())), preferred_element_type=f32)


def softplus(z):
    return jnp.maximum(z, 0.0) + jnp.log(1.0 + jnp.exp(-jnp.abs(z)))


def kernel(
    n_sp,
    n_out,
    tok_ref,
    gain_ref,
    gatew_ref,
    bias_ref,
    shift_ref,
    sbias_ref,
    mgain_ref,
    sgain_ref,
    wk_hbm,
    wv_hbm,
    wq_hbm,
    wo_hbm,
    sq_hbm,
    sk_hbm,
    sv_hbm,
    om_hbm,
    os_hbm,
    out_ref,
    tok_in,
    nrm,
    xg,
    wm,
    ws,
    wout,
    sb1,
    rb1,
    sb2,
    rb2,
    proj,
    squery,
    kv,
    stick_acc,
    stick_run,
    gates,
    state_own,
    state_in,
    state_out,
    log_in,
    log_out,
    mix,
    ob,
    orb,
    load_sem,
    tok_s,
    tok_r,
    a2a_s,
    a2a_r,
    fwd_s,
    fwd_r,
    st1_s,
    st1_r,
    st2_s,
    st2_r,
    kv_s,
    kv_r,
    chain_s,
    chain_r,
    log_s,
    log_r,
    out_s,
    out_r,
):
    f = lax.axis_index("fs")
    s = lax.axis_index("sp")
    t = lax.axis_index("tp")
    rows, half_feat = tok_ref.shape
    heads = state_own.shape[0]
    dm = state_own.shape[1]
    ds = sgain_ref.shape[1] // heads
    block = wm.shape[1]
    half = rows // 2
    other = 1 - t

    def flip(bits):
        if bits == 3:
            return 3 - f
        if bits == 1:
            return f + 1 - 2 * (f % 2)
        return f + 2 - 4 * (f // 2)

    def remote(src, dst, send, recv, device):
        return pltpu.make_async_remote_copy(
            src_ref=src,
            dst_ref=dst,
            send_sem=send,
            recv_sem=recv,
            device_id=device,
            device_id_type=MESH,
        )

    width_s = ws.shape[2]
    loads = [
        pltpu.make_async_copy(sq_hbm, ws.at[0], load_sem.at[0]),
        pltpu.make_async_copy(sk_hbm, ws.at[1], load_sem.at[1]),
        pltpu.make_async_copy(sv_hbm, ws.at[2], load_sem.at[2]),
        pltpu.make_async_copy(wk_hbm, wm.at[0], load_sem.at[3]),
        pltpu.make_async_copy(wv_hbm, wm.at[1], load_sem.at[4]),
        pltpu.make_async_copy(wq_hbm, wm.at[2], load_sem.at[5]),
        pltpu.make_async_copy(wo_hbm, wm.at[3], load_sem.at[6]),
        pltpu.make_async_copy(om_hbm, wout.at[pl.ds(0, heads * dm)], load_sem.at[7]),
        pltpu.make_async_copy(os_hbm, wout.at[pl.ds(heads * dm, heads * ds)], load_sem.at[8]),
    ]
    for load in loads:
        load.start()

    barrier = pltpu.get_barrier_semaphore()
    pl.semaphore_signal(barrier, inc=1, device_id={"tp": other}, device_id_type=MESH)
    for bits in (1, 2, 3):
        pl.semaphore_signal(barrier, inc=1, device_id={"fs": flip(bits)}, device_id_type=MESH)

    @pl.when(s > 0)
    def _():
        pl.semaphore_signal(barrier, inc=1, device_id={"sp": s - 1}, device_id_type=MESH)

    @pl.when(s < n_sp - 1)
    def _():
        pl.semaphore_signal(barrier, inc=1, device_id={"sp": s + 1}, device_id_type=MESH)

    peers = 4 + jnp.where(s > 0, 1, 0) + jnp.where(s < n_sp - 1, 1, 0)
    pl.semaphore_wait(barrier, peers)

    tok_copy = remote(tok_ref, tok_in, tok_s.at[0], tok_r.at[0], {"tp": other})
    tok_copy.start()
    tok_copy.wait_recv()

    step_rows = 32
    own_cols = pl.ds(pl.multiple_of(t * half_feat, half_feat), half_feat)
    far_cols = pl.ds(pl.multiple_of(other * half_feat, half_feat), half_feat)

    def norm_rows(i, _):
        at = pl.ds(pl.multiple_of(i * step_rows, step_rows), step_rows)
        own = tok_ref[at, :].astype(f32)
        far = tok_in[at, :].astype(f32)
        total = jnp.sum(own * own, axis=1, keepdims=True) + jnp.sum(far * far, axis=1, keepdims=True)
        scale = lax.rsqrt(total / (2 * half_feat) + epsilon)
        nrm[at, own_cols] = (own * scale * gain_ref[:, own_cols]).astype(bf16)
        nrm[at, far_cols] = (far * scale * gain_ref[:, far_cols]).astype(bf16)
        return 0

    lax.fori_loop(0, rows // step_rows, norm_rows, 0)

    my_rows = pl.ds(pl.multiple_of(t * half, half), half)
    a2a, fwd = {}, {}
    for bits in (3, 1, 2):
        to = flip(bits)
        a2a[bits] = remote(
            nrm.at[my_rows, pl.ds(pl.multiple_of(to * block, block), block)],
            xg.at[bits, my_rows],
            a2a_s.at[bits - 1],
            a2a_r.at[bits - 1],
            {"fs": to},
        )
        a2a[bits].start()

    for load in loads[:3]:
        load.wait()
    normed = nrm[...]
    kv[0, 0] = dot(normed, ws[1]).astype(bf16)
    kv[0, 1] = dot(normed, ws[2]).astype(bf16)

    def kv_copy(d):
        return remote(kv.at[d - 1], kv.at[d], kv_s.at[d], kv_r.at[d], {"sp": s + 1})

    def kv_send(d):
        @pl.when((s < n_sp - 1) & (s >= d - 1))
        def _():
            kv_copy(d).start()

    kv_send(1)
    squery[...] = dot(normed, ws[0]).astype(bf16)
    xg[0] = nrm[:, pl.ds(pl.multiple_of(f * block, block), block)]

    for bits in (1, 2, 3):
        a2a[bits].wait_recv()
        fwd[bits] = remote(
            xg.at[bits, my_rows],
            xg.at[bits, my_rows],
            fwd_s.at[bits - 1],
            fwd_r.at[bits - 1],
            {"tp": other},
        )
        fwd[bits].start()
    for load in loads[3:]:
        load.wait()
    for bits in (1, 2, 3):
        fwd[bits].wait_recv()

    def order(h):
        return (1, 2) if h % 2 == 0 else (2, 1)

    def partial(p, h, seq):
        return dot(xg[seq], wm[p, :, h * dm : (h + 1) * dm])

    def first_copy(p, h, which):
        at = (p * heads + h) * 2 + which
        return remote(
            sb1.at[p, h, which], rb1.at[p, h, which], st1_s.at[at], st1_r.at[at],
            {"fs": flip(order(h)[0])},
        )

    def second_copy(p, h):
        at = p * heads + h
        return remote(
            sb2.at[p, h], rb2.at[p, h], st2_s.at[at], st2_r.at[at], {"fs": flip(order(h)[1])}
        )

    def first_step(p):
        for which, bits in ((1, 3), (0, None)):
            for h in range(heads):
                sb1[p, h, which] = partial(p, h, bits or order(h)[0]).astype(bf16)
                first_copy(p, h, which).start()

    def second_step(p):
        for h in range(heads):
            mine = partial(p, h, order(h)[1])
            first_copy(p, h, 1).wait_recv()
            sb2[p, h] = (mine + rb1[p, h, 1].astype(f32)).astype(bf16)
            second_copy(p, h).start()

    def finish(p, h):
        mine = partial(p, h, 0)
        first_copy(p, h, 0).wait_recv()
        second_copy(p, h).wait_recv()
        return (mine + rb1[p, h, 0].astype(f32) + rb2[p, h].astype(f32)).astype(bf16)

    for p in range(4):
        first_step(p)

    row_at = lax.broadcasted_iota(jnp.int32, (rows, rows), 0)
    col_at = lax.broadcasted_iota(jnp.int32, (rows, rows), 1)
    gate = dot(nrm[...], gatew_ref[...])
    log_forget = shift_ref[...] - softplus(-(gate + bias_ref[...]))
    tril = (row_at >= col_at).astype(f32)
    cumulative = lax.dot_general(
        tril, log_forget, (((1,), (0,)), ((), ())),
        precision=lax.Precision.HIGHEST, preferred_element_type=f32,
    )
    gates[0] = gate
    gates[1] = cumulative

    def stick_part(h, kv_at, diagonal):
        cols = slice(h * ds, (h + 1) * ds)
        z = dot(squery[:, cols], kv[kv_at, 0, :, cols], ((1,), (1,)))
        z = z * ds ** (-0.5) + sbias_ref[h]
        keep = -softplus(z)
        visible = col_at < row_at
        if diagonal:
            kept = jnp.where(visible, keep, 0.0)
        else:
            kept = keep
        strict = (row_at > col_at).astype(bf16)
        high = kept.astype(bf16)
        low = (kept - high.astype(f32)).astype(bf16)
        after = dot(high, strict) + dot(low, strict)
        weights = jnp.exp(z + keep + after)
        if diagonal:
            weights = jnp.where(visible, weights, 0.0)
        part = dot(weights.astype(bf16), kv[kv_at, 1, :, cols])
        return part, jnp.sum(kept, axis=1, keepdims=True)

    def stick_own():
        for h in range(heads):
            part, keep = stick_part(h, 0, True)
            stick_acc[h] = part
            stick_run[h] = jnp.broadcast_to(keep, stick_run.shape[1:])

    def stick_span(d):
        @pl.when(s >= d)
        def _():
            remote(kv.at[d - 1], kv.at[d], kv_s.at[d], kv_r.at[d], {"sp": s - 1}).wait_recv()

        kv_next(d)

        @pl.when(s >= d)
        def _():
            for h in range(heads):
                part, keep = stick_part(h, d, False)
                stick_acc[h] = stick_acc[h] + jnp.exp(stick_run[h]) * part
                stick_run[h] = stick_run[h] + keep

    def kv_next(d):
        @pl.when((s < n_sp - 1) & (s >= d) & (d < n_sp - 1))
        def _():
            kv_copy(d + 1).start()

    def stick_spans(low, high):
        if high > low:
            lax.fori_loop(low, high, lambda d, c: (stick_span(d), c)[1], 0)

    stick_own()
    second_step(KEY)
    stick_spans(1, min(2, n_sp))
    second_step(VALUE)

    def column(h):
        return gates[0, :, h : h + 1] - gates[1, :, heads + h : heads + h + 1]

    for h in range(heads):
        proj[KEY, h] = (finish(KEY, h).astype(f32) * dm ** (-0.5)).astype(bf16)
        proj[VALUE, h] = finish(VALUE, h)
        u = column(h)
        top = jnp.max(u, axis=0, keepdims=True)
        weighted = (proj[KEY, h].astype(f32) * jnp.exp(u - top)).astype(bf16)
        state_own[h] = dot(weighted, proj[VALUE, h], ((0,), (0,)))

    def log_copy(to):
        return remote(log_out, log_in, log_s.at[0], log_r.at[0], {"sp": to})

    def chain_copy(h, to):
        return remote(state_out.at[h], state_in.at[h], chain_s.at[h], chain_r.at[h], {"sp": to})

    def chain():
        @pl.when(s == 0)
        def _():
            log_in[...] = jnp.full(log_in.shape, floor_neg, f32)
            state_in[...] = jnp.zeros(state_in.shape, bf16)

        @pl.when(s > 0)
        def _():
            log_copy(s - 1).wait_recv()

        factors = []
        for h in range(heads):
            total = gates[1, rows - 1 : rows, heads + h : heads + h + 1]
            early = total + log_in[h : h + 1, 0:1]
            late = total + jnp.max(column(h), axis=0, keepdims=True)
            top = jnp.maximum(early, late)
            log_out[h : h + 1, :] = jnp.broadcast_to(top, (1, log_out.shape[1]))
            factors.append((jnp.exp(early - top), jnp.exp(late - top)))

        @pl.when(s < n_sp - 1)
        def _():
            log_copy(s + 1).start()

        for h in range(heads):

            @pl.when(s > 0)
            def _():
                chain_copy(h, s - 1).wait_recv()

            @pl.when(s < n_sp - 1)
            def _():
                early, late = factors[h]
                state_out[h] = (early * state_in[h].astype(f32) + late * state_own[h]).astype(bf16)
                chain_copy(h, s + 1).start()

    log_out[...] = jnp.zeros(log_out.shape, f32)
    pl.when(s == 0)(chain)
    second_step(QUERY)
    stick_spans(2, min(3, n_sp))
    pl.when(s == 1)(chain)
    second_step(GATE)
    stick_spans(3, n_sp)

    for h in range(heads):
        cols = slice(h * ds, (h + 1) * ds)
        out = stick_acc[h]
        scale = lax.rsqrt(jnp.mean(out * out, axis=1, keepdims=True) + epsilon)
        mix[:, heads * dm + h * ds : heads * dm + (h + 1) * ds] = (
            out * scale * sgain_ref[:, cols]
        ).astype(bf16)

    for h in range(heads):
        proj[QUERY, h] = finish(QUERY, h)
    pl.when(s > 1)(chain)

    gate_rows = jnp.transpose(gates[0] - pltpu.roll(gates[1], gates.shape[2] - heads, 1))
    causal = col_at <= row_at
    for h in range(heads):
        u_row = gate_rows[h : h + 1, :]
        carried_max = log_in[h : h + 1, 0:1]
        masked = jnp.where(causal, u_row, floor_neg)
        running = jnp.maximum(carried_max, jnp.max(masked, axis=1, keepdims=True))
        carried = jnp.exp(carried_max - running)
        queries = proj[QUERY, h]
        scores = dot(queries, proj[KEY, h], ((1,), (1,))) * jnp.exp(masked - running)
        memory = carried * dot(queries, state_in[h]) + dot(scores.astype(bf16), proj[VALUE, h])
        gated = memory / (1.0 + jnp.exp(-finish(GATE, h).astype(f32)))
        scale = lax.rsqrt(jnp.mean(gated * gated, axis=1, keepdims=True) + epsilon)
        cols = slice(h * dm, (h + 1) * dm)
        mix[:, cols] = (gated * scale * mgain_ref[:, cols]).astype(bf16)

    piece = wout.shape[1] // n_out
    far_rows = pl.ds(pl.multiple_of(other * half, half), half)
    copies = []
    for c in range(n_out):
        cols = slice(c * piece, (c + 1) * piece)
        ob[c] = dot(mix[far_rows, :], wout[:, cols]).astype(bf16)
        copy = remote(ob.at[c], orb.at[c], out_s.at[c], out_r.at[c], {"tp": other})
        copy.start()
        copies.append(copy)
    for c in range(n_out):
        cols = slice(c * piece, (c + 1) * piece)
        mine = dot(mix[my_rows, :], wout[:, cols])
        copies[c].wait_recv()
        out_ref[:, cols] = (mine + orb[c].astype(f32)).astype(bf16)

    tok_copy.wait_send()
    for bits in (1, 2, 3):
        a2a[bits].wait_send()
        fwd[bits].wait_send()
    for p in range(4):
        for h in range(heads):
            first_copy(p, h, 0).wait_send()
            first_copy(p, h, 1).wait_send()
            second_copy(p, h).wait_send()
    for copy in copies:
        copy.wait_send()

    @pl.when(s < n_sp - 1)
    def _():
        log_copy(s + 1).wait_send()
        for h in range(heads):
            chain_copy(h, s + 1).wait_send()

    def kv_done(d, c):
        @pl.when((s < n_sp - 1) & (s >= d - 1))
        def _():
            kv_copy(d).wait_send()

        return c

    if n_sp > 1:
        lax.fori_loop(1, n_sp, kv_done, 0)


def per_device(
    n_sp,
    tokens,
    norm_gain,
    memory_query,
    memory_key,
    memory_value,
    memory_outgate,
    memory_ingate,
    memory_forget,
    forget_bias,
    forget_shift,
    stick_query,
    stick_key,
    stick_value,
    stick_bias,
    memory_gain,
    stick_gain,
    out_memory,
    out_stick,
):
    rows, half_feat = tokens.shape[1:]
    features = 2 * half_feat
    heads = forget_bias.shape[0]
    block, width = memory_query.shape
    dm = width // heads
    stick_width = stick_query.shape[1]
    ds = stick_width // heads
    lanes = 128
    n_out = 4
    half = rows // 2

    gate_weight = jnp.pad(
        jnp.concatenate([memory_ingate, memory_forget], axis=1), ((0, 0), (0, lanes - 2 * heads))
    )
    bias = jnp.pad(forget_bias[None], ((0, 0), (heads, lanes - 2 * heads)))
    shift = jnp.pad(forget_shift[0], ((0, 0), (heads, lanes - 2 * heads)))

    vmem = pl.BlockSpec(memory_space=pltpu.VMEM)
    smem = pl.BlockSpec(memory_space=pltpu.SMEM)
    anyw = pl.BlockSpec(memory_space=pl.ANY)
    dma = pltpu.SemaphoreType.DMA
    out = pl.pallas_call(
        functools.partial(kernel, n_sp, n_out),
        out_shape=jax.ShapeDtypeStruct((half, features), bf16),
        in_specs=[vmem] * 5 + [smem] + [vmem] * 2 + [anyw] * 9,
        out_specs=vmem,
        scratch_shapes=[
            pltpu.VMEM((rows, half_feat), bf16),
            pltpu.VMEM((rows, features), bf16),
            pltpu.VMEM((4, rows, block), bf16),
            pltpu.VMEM((4, block, width), bf16),
            pltpu.VMEM((3, features, stick_width), bf16),
            pltpu.VMEM((width + stick_width, features), bf16),
            pltpu.VMEM((4, heads, 2, rows, dm), bf16),
            pltpu.VMEM((4, heads, 2, rows, dm), bf16),
            pltpu.VMEM((4, heads, rows, dm), bf16),
            pltpu.VMEM((4, heads, rows, dm), bf16),
            pltpu.VMEM((4, heads, rows, dm), bf16),
            pltpu.VMEM((rows, stick_width), bf16),
            pltpu.VMEM((n_sp, 2, rows, stick_width), bf16),
            pltpu.VMEM((heads, rows, ds), f32),
            pltpu.VMEM((heads, rows, ds), f32),
            pltpu.VMEM((2, rows, lanes), f32),
            pltpu.VMEM((heads, dm, dm), f32),
            pltpu.VMEM((heads, dm, dm), bf16),
            pltpu.VMEM((heads, dm, dm), bf16),
            pltpu.VMEM((8, lanes), f32),
            pltpu.VMEM((8, lanes), f32),
            pltpu.VMEM((rows, width + stick_width), bf16),
            pltpu.VMEM((n_out, half, features // n_out), bf16),
            pltpu.VMEM((n_out, half, features // n_out), bf16),
            dma((9,)),
            dma((1,)),
            dma((1,)),
            dma((3,)),
            dma((3,)),
            dma((3,)),
            dma((3,)),
            dma((8 * heads,)),
            dma((8 * heads,)),
            dma((4 * heads,)),
            dma((4 * heads,)),
            dma((n_sp,)),
            dma((n_sp,)),
            dma((heads,)),
            dma((heads,)),
            dma((1,)),
            dma((1,)),
            dma((n_out,)),
            dma((n_out,)),
        ],
        compiler_params=pltpu.CompilerParams(
            collective_id=0, has_side_effects=True, vmem_limit_bytes=60 * 1024 * 1024
        ),
    )(
        tokens[0],
        norm_gain[None],
        gate_weight,
        bias,
        shift,
        stick_bias,
        memory_gain[None],
        stick_gain[None],
        memory_key,
        memory_value,
        memory_query,
        memory_outgate,
        stick_query,
        stick_key,
        stick_value,
        out_memory,
        out_stick,
    )
    return out[None]


def solution(mesh):
    assert mesh.shape["fs"] == 4 and mesh.shape["tp"] == 2
    return jax.shard_map(
        functools.partial(per_device, mesh.shape["sp"]),
        mesh=mesh,
        in_specs=(
            P("fs", "sp", "tp"),
            P(),
            P("fs", "tp"),
            P("fs", "tp"),
            P("fs", "tp"),
            P("fs", "tp"),
            P(None, "tp"),
            P(None, "tp"),
            P("tp"),
            P("fs", "sp", "tp"),
            P(None, "tp"),
            P(None, "tp"),
            P(None, "tp"),
            P("tp"),
            P("tp"),
            P("tp"),
            P("tp", None),
            P("tp", None),
        ),
        out_specs=P("fs", ("sp", "tp"), None),
        check_vma=False,
    )
```

```python
import functools

import jax
import jax.numpy as jnp
from jax import lax
from jax.experimental import pallas as pl
from jax.experimental.pallas import tpu as pltpu
from jax.sharding import PartitionSpec as P

MESH = pl.DeviceIdType.MESH
epsilon = 1e-06
floor_neg = -1e30
f32 = jnp.float32
bf16 = jnp.bfloat16

KEY, VALUE, QUERY, GATE = 0, 1, 2, 3


def dot(a, b, dims=((1,), (0,))):
    return lax.dot_general(a, b, (dims, ((), ())), preferred_element_type=f32)


def softplus(z):
    return jnp.maximum(z, 0.0) + jnp.log(1.0 + jnp.exp(-jnp.abs(z)))


def kernel(
    n_sp,
    n_out,
    tok_ref,
    gain_ref,
    ingate_ref,
    forget_ref,
    bias_ref,
    shift_ref,
    sbias_ref,
    mgain_ref,
    sgain_ref,
    wk_hbm,
    wv_hbm,
    wq_hbm,
    wo_hbm,
    sq_hbm,
    sk_hbm,
    sv_hbm,
    om_hbm,
    os_hbm,
    out_ref,
    tok_in,
    nrm,
    xg,
    wm,
    wg,
    ws,
    wout,
    sb,
    rb,
    own_part,
    proj,
    squery,
    kv,
    stick_acc,
    stick_run,
    gw,
    u_rows,
    u_cols,
    totals,
    state_own,
    state_in,
    state_out,
    log_in,
    log_out,
    mix,
    ob,
    orb,
    load_sem,
    tok_s,
    tok_r,
    a2a_s,
    a2a_r,
    fwd_s,
    fwd_r,
    w_s,
    w_r,
    rs_s,
    rs_r,
    kv_s,
    kv_r,
    chain_s,
    chain_r,
    log_s,
    log_r,
    out_s,
    out_r,
):
    f = lax.axis_index("fs")
    s = lax.axis_index("sp")
    t = lax.axis_index("tp")
    rows, half_feat = tok_ref.shape
    heads = state_own.shape[0]
    dm = state_own.shape[1]
    ds = sgain_ref.shape[1] // heads
    block = wm.shape[1]
    half = rows // 2
    other = 1 - t

    def flip(bits):
        if bits == 3:
            return 3 - f
        if bits == 1:
            return f + 1 - 2 * (f % 2)
        return f + 2 - 4 * (f // 2)

    def remote(src, dst, send, recv, device):
        return pltpu.make_async_remote_copy(
            src_ref=src,
            dst_ref=dst,
            send_sem=send,
            recv_sem=recv,
            device_id=device,
            device_id_type=MESH,
        )

    width_s = ws.shape[2]
    loads = [
        pltpu.make_async_copy(sq_hbm, ws.at[0], load_sem.at[0]),
        pltpu.make_async_copy(sk_hbm, ws.at[1], load_sem.at[1]),
        pltpu.make_async_copy(sv_hbm, ws.at[2], load_sem.at[2]),
        pltpu.make_async_copy(wk_hbm, wm.at[0], load_sem.at[3]),
        pltpu.make_async_copy(wv_hbm, wm.at[1], load_sem.at[4]),
        pltpu.make_async_copy(wq_hbm, wm.at[2], load_sem.at[5]),
        pltpu.make_async_copy(wo_hbm, wm.at[3], load_sem.at[6]),
        pltpu.make_async_copy(om_hbm, wout.at[pl.ds(0, heads * dm)], load_sem.at[7]),
        pltpu.make_async_copy(os_hbm, wout.at[pl.ds(heads * dm, heads * ds)], load_sem.at[8]),
    ]
    for load in loads:
        load.start()

    barrier = pltpu.get_barrier_semaphore()
    pl.semaphore_signal(barrier, inc=1, device_id={"tp": other}, device_id_type=MESH)
    for bits in (1, 2, 3):
        pl.semaphore_signal(barrier, inc=1, device_id={"fs": flip(bits)}, device_id_type=MESH)

    @pl.when(s > 0)
    def _():
        pl.semaphore_signal(barrier, inc=1, device_id={"sp": s - 1}, device_id_type=MESH)

    @pl.when(s < n_sp - 1)
    def _():
        pl.semaphore_signal(barrier, inc=1, device_id={"sp": s + 1}, device_id_type=MESH)

    peers = 4 + jnp.where(s > 0, 1, 0) + jnp.where(s < n_sp - 1, 1, 0)
    pl.semaphore_wait(barrier, peers)

    tok_copy = remote(tok_ref, tok_in, tok_s.at[0], tok_r.at[0], {"tp": other})
    tok_copy.start()

    def pair_bits(h):
        return 1 if h % 2 == 0 else 2

    def sum_bits(h):
        return 3 - pair_bits(h)

    def weight_copy(p, h):
        at = p * heads + h
        return remote(
            wm.at[p, :, pl.ds(h * dm, dm)], wg.at[p, h], w_s.at[at], w_r.at[at],
            {"fs": flip(pair_bits(h))},
        )

    def send_weight(p):
        loads[3 + p].wait()
        for h in range(heads):
            weight_copy(p, h).start()

    send_weight(KEY)
    tok_copy.wait_recv()

    step_rows = 32
    own_cols = pl.ds(pl.multiple_of(t * half_feat, half_feat), half_feat)
    far_cols = pl.ds(pl.multiple_of(other * half_feat, half_feat), half_feat)

    def norm_rows(i, _):
        at = pl.ds(pl.multiple_of(i * step_rows, step_rows), step_rows)
        own = tok_ref[at, :].astype(f32)
        far = tok_in[at, :].astype(f32)
        total = jnp.sum(own * own, axis=1, keepdims=True) + jnp.sum(far * far, axis=1, keepdims=True)
        scale = lax.rsqrt(total / (2 * half_feat) + epsilon)
        nrm[at, own_cols] = (own * scale * gain_ref[:, own_cols]).astype(bf16)
        nrm[at, far_cols] = (far * scale * gain_ref[:, far_cols]).astype(bf16)
        return 0

    lax.fori_loop(0, rows // step_rows, norm_rows, 0)

    my_rows = pl.ds(pl.multiple_of(t * half, half), half)

    def feature_block(index):
        return pl.ds(pl.multiple_of(index * block, block), block)

    a2a, fwd = {}, {}
    for h in range(heads):
        for which in range(2):
            at = h * 2 + which
            to = flip(sum_bits(h))
            a2a[at] = remote(
                nrm.at[my_rows, feature_block(to if which == 0 else flip(3))],
                xg.at[h, which, my_rows],
                a2a_s.at[at],
                a2a_r.at[at],
                {"fs": to},
            )
            a2a[at].start()
    send_weight(VALUE)

    for load in loads[:3]:
        load.wait()
    normed = nrm[...]
    kv[0, 0] = dot(normed, ws[1]).astype(bf16)
    kv[0, 1] = dot(normed, ws[2]).astype(bf16)

    def kv_copy(d):
        return remote(kv.at[d - 1], kv.at[d], kv_s.at[d], kv_r.at[d], {"sp": s + 1})

    def kv_send(d):
        @pl.when((s < n_sp - 1) & (s >= d - 1))
        def _():
            kv_copy(d).start()

    kv_send(1)
    squery[...] = dot(normed, ws[0]).astype(bf16)

    row_at = lax.broadcasted_iota(jnp.int32, (rows, rows), 0)
    col_at = lax.broadcasted_iota(jnp.int32, (rows, rows), 1)
    gw[...] = jnp.zeros(gw.shape, bf16)
    gw[0:heads, :] = ingate_ref[...]
    gw[8 : 8 + heads, :] = forget_ref[...]
    gate = dot(gw[...], normed, ((1,), (1,)))
    triu = (row_at <= col_at).astype(f32)
    u_rows[...] = jnp.zeros(u_rows.shape, f32)
    for h in range(heads):
        log_forget = shift_ref[h : h + 1, :] - softplus(-(gate[8 + h : 9 + h, :] + bias_ref[h]))
        cumulative = lax.dot_general(
            jnp.broadcast_to(log_forget, (8, rows)), triu, (((1,), (0,)), ((), ())),
            precision=lax.Precision.HIGHEST, preferred_element_type=f32,
        )
        u_rows[h : h + 1, :] = gate[h : h + 1, :] - cumulative[0:1, :]
        totals[h : h + 1, :] = jnp.broadcast_to(
            cumulative[0:1, rows - 1 : rows], (1, totals.shape[1])
        )
    u_cols[...] = jnp.transpose(u_rows[...])

    def stick_part(h, kv_at, diagonal):
        cols = slice(h * ds, (h + 1) * ds)
        z = dot(squery[:, cols], kv[kv_at, 0, :, cols], ((1,), (1,)))
        z = z * ds ** (-0.5) + sbias_ref[h]
        keep = -softplus(z)
        visible = col_at < row_at
        if diagonal:
            kept = jnp.where(visible, keep, 0.0)
        else:
            kept = keep
        strict = (row_at > col_at).astype(bf16)
        high = kept.astype(bf16)
        low = (kept - high.astype(f32)).astype(bf16)
        after = dot(high, strict) + dot(low, strict)
        weights = jnp.exp(z + keep + after)
        if diagonal:
            weights = jnp.where(visible, weights, 0.0)
        part = dot(weights.astype(bf16), kv[kv_at, 1, :, cols])
        return part, jnp.sum(kept, axis=1, keepdims=True)

    def stick_own():
        for h in range(heads):
            part, keep = stick_part(h, 0, True)
            stick_acc[h] = part
            stick_run[h] = jnp.broadcast_to(keep, stick_run.shape[1:])

    def stick_span(d):
        @pl.when(s >= d)
        def _():
            remote(kv.at[d - 1], kv.at[d], kv_s.at[d], kv_r.at[d], {"sp": s - 1}).wait_recv()

        kv_next(d)

        @pl.when(s >= d)
        def _():
            for h in range(heads):
                part, keep = stick_part(h, d, False)
                stick_acc[h] = stick_acc[h] + jnp.exp(stick_run[h]) * part
                stick_run[h] = stick_run[h] + keep

    def kv_next(d):
        @pl.when((s < n_sp - 1) & (s >= d) & (d < n_sp - 1))
        def _():
            kv_copy(d + 1).start()

    def stick_spans(low, high):
        if high > low:
            lax.fori_loop(low, high, lambda d, c: (stick_span(d), c)[1], 0)

    stick_own()
    for at in range(2 * heads):
        a2a[at].wait_recv()
        h, which = divmod(at, 2)
        fwd[at] = remote(
            xg.at[h, which, my_rows],
            xg.at[h, which, my_rows],
            fwd_s.at[at],
            fwd_r.at[at],
            {"tp": other},
        )
        fwd[at].start()

    def rs_copy(p, h):
        at = p * heads + h
        return remote(
            sb.at[p, h], rb.at[p, h], rs_s.at[at], rs_r.at[at], {"fs": flip(sum_bits(h))}
        )

    def partials(p):
        for h in range(heads):
            cols = slice(h * dm, (h + 1) * dm)
            if p == KEY:
                fwd[2 * h].wait_recv()
                fwd[2 * h + 1].wait_recv()
            weight_copy(p, h).wait_recv()
            sb[p, h] = (dot(xg[h, 0], wm[p, :, cols]) + dot(xg[h, 1], wg[p, h])).astype(bf16)
            rs_copy(p, h).start()

    def own_partials(p):
        for h in range(heads):
            cols = slice(h * dm, (h + 1) * dm)
            own_part[p, h] = dot(nrm[:, feature_block(f)], wm[p, :, cols]) + dot(
                nrm[:, feature_block(flip(pair_bits(h)))], wg[p, h]
            )

    def finish(p, h):
        rs_copy(p, h).wait_recv()
        return (own_part[p, h] + rb[p, h].astype(f32)).astype(bf16)

    partials(KEY)
    own_partials(KEY)
    partials(VALUE)
    send_weight(QUERY)
    send_weight(GATE)
    own_partials(VALUE)
    stick_spans(1, min(2, n_sp))

    def column(h):
        return u_cols[:, h : h + 1]

    for h in range(heads):
        proj[KEY, h] = (finish(KEY, h).astype(f32) * dm ** (-0.5)).astype(bf16)
        proj[VALUE, h] = finish(VALUE, h)
        u = column(h)
        top = jnp.max(u, axis=0, keepdims=True)
        weighted = (proj[KEY, h].astype(f32) * jnp.exp(u - top)).astype(bf16)
        state_own[h] = dot(weighted, proj[VALUE, h], ((0,), (0,)))

    def log_copy(to):
        return remote(log_out, log_in, log_s.at[0], log_r.at[0], {"sp": to})

    piece_dm = dm // 2

    def chain_copy(h, c, to):
        cols = pl.ds(c * piece_dm, piece_dm)
        at = h * 2 + c
        return remote(
            state_out.at[h, :, cols], state_in.at[h, :, cols], chain_s.at[at], chain_r.at[at],
            {"sp": to},
        )

    def chain():
        @pl.when(s == 0)
        def _():
            log_in[...] = jnp.full(log_in.shape, floor_neg, f32)
            state_in[...] = jnp.zeros(state_in.shape, bf16)

        @pl.when(s > 0)
        def _():
            log_copy(s - 1).wait_recv()

        factors = []
        for h in range(heads):
            total = totals[h : h + 1, 0:1]
            early = total + log_in[h : h + 1, 0:1]
            late = total + jnp.max(column(h), axis=0, keepdims=True)
            top = jnp.maximum(early, late)
            log_out[h : h + 1, :] = jnp.broadcast_to(top, (1, log_out.shape[1]))
            factors.append((jnp.exp(early - top), jnp.exp(late - top)))

        @pl.when(s < n_sp - 1)
        def _():
            log_copy(s + 1).start()

        for at in range(2 * heads):
            h, c = divmod(at, 2)
            cols = slice(c * piece_dm, (c + 1) * piece_dm)

            @pl.when(s > 0)
            def _():
                chain_copy(h, c, s - 1).wait_recv()

            @pl.when(s < n_sp - 1)
            def _():
                early, late = factors[h]
                state_out[h, :, cols] = (
                    early * state_in[h, :, cols].astype(f32) + late * state_own[h, :, cols]
                ).astype(bf16)
                chain_copy(h, c, s + 1).start()

    log_out[...] = jnp.zeros(log_out.shape, f32)
    pl.when(s == 0)(chain)
    stick_spans(2, min(3, n_sp))
    partials(QUERY)
    pl.when(s == 1)(chain)
    own_partials(QUERY)
    pl.when(s == 2)(chain)
    partials(GATE)
    own_partials(GATE)
    stick_spans(3, n_sp)
    for load in loads[7:]:
        load.wait()

    for h in range(heads):
        cols = slice(h * ds, (h + 1) * ds)
        out = stick_acc[h]
        scale = lax.rsqrt(jnp.mean(out * out, axis=1, keepdims=True) + epsilon)
        mix[:, heads * dm + h * ds : heads * dm + (h + 1) * ds] = (
            out * scale * sgain_ref[:, cols]
        ).astype(bf16)

    for h in range(heads):
        proj[QUERY, h] = finish(QUERY, h)
    pl.when(s > 2)(chain)

    causal = col_at <= row_at
    for h in range(heads):
        u_row = u_rows[h : h + 1, :]
        carried_max = log_in[h : h + 1, 0:1]
        masked = jnp.where(causal, u_row, floor_neg)
        running = jnp.maximum(carried_max, jnp.max(masked, axis=1, keepdims=True))
        carried = jnp.exp(carried_max - running)
        queries = proj[QUERY, h]
        scores = dot(queries, proj[KEY, h], ((1,), (1,))) * jnp.exp(masked - running)
        memory = carried * dot(queries, state_in[h]) + dot(scores.astype(bf16), proj[VALUE, h])
        gated = memory / (1.0 + jnp.exp(-finish(GATE, h).astype(f32)))
        scale = lax.rsqrt(jnp.mean(gated * gated, axis=1, keepdims=True) + epsilon)
        cols = slice(h * dm, (h + 1) * dm)
        mix[:, cols] = (gated * scale * mgain_ref[:, cols]).astype(bf16)

    piece = wout.shape[1] // n_out
    far_rows = pl.ds(pl.multiple_of(other * half, half), half)
    copies = []
    for c in range(n_out):
        cols = slice(c * piece, (c + 1) * piece)
        ob[c] = dot(mix[far_rows, :], wout[:, cols]).astype(bf16)
        copy = remote(ob.at[c], orb.at[c], out_s.at[c], out_r.at[c], {"tp": other})
        copy.start()
        copies.append(copy)
    for c in range(n_out):
        cols = slice(c * piece, (c + 1) * piece)
        mine = dot(mix[my_rows, :], wout[:, cols])
        copies[c].wait_recv()
        out_ref[:, cols] = (mine + orb[c].astype(f32)).astype(bf16)

    tok_copy.wait_send()
    for at in range(2 * heads):
        a2a[at].wait_send()
        fwd[at].wait_send()
    for p in range(4):
        for h in range(heads):
            weight_copy(p, h).wait_send()
            rs_copy(p, h).wait_send()
    for copy in copies:
        copy.wait_send()

    @pl.when(s < n_sp - 1)
    def _():
        log_copy(s + 1).wait_send()
        for at in range(2 * heads):
            chain_copy(at // 2, at % 2, s + 1).wait_send()

    def kv_done(d, c):
        @pl.when((s < n_sp - 1) & (s >= d - 1))
        def _():
            kv_copy(d).wait_send()

        return c

    if n_sp > 1:
        lax.fori_loop(1, n_sp, kv_done, 0)


def per_device(
    n_sp,
    tokens,
    norm_gain,
    memory_query,
    memory_key,
    memory_value,
    memory_outgate,
    memory_ingate,
    memory_forget,
    forget_bias,
    forget_shift,
    stick_query,
    stick_key,
    stick_value,
    stick_bias,
    memory_gain,
    stick_gain,
    out_memory,
    out_stick,
):
    rows, half_feat = tokens.shape[1:]
    features = 2 * half_feat
    heads = forget_bias.shape[0]
    block, width = memory_query.shape
    dm = width // heads
    stick_width = stick_query.shape[1]
    ds = stick_width // heads
    lanes = 128
    n_out = 4
    half = rows // 2

    vmem = pl.BlockSpec(memory_space=pltpu.VMEM)
    smem = pl.BlockSpec(memory_space=pltpu.SMEM)
    anyw = pl.BlockSpec(memory_space=pl.ANY)
    dma = pltpu.SemaphoreType.DMA
    out = pl.pallas_call(
        functools.partial(kernel, n_sp, n_out),
        out_shape=jax.ShapeDtypeStruct((half, features), bf16),
        in_specs=[vmem] * 4 + [smem, vmem, smem] + [vmem] * 2 + [anyw] * 9,
        out_specs=vmem,
        scratch_shapes=[
            pltpu.VMEM((rows, half_feat), bf16),
            pltpu.VMEM((rows, features), bf16),
            pltpu.VMEM((heads, 2, rows, block), bf16),
            pltpu.VMEM((4, block, width), bf16),
            pltpu.VMEM((4, heads, block, dm), bf16),
            pltpu.VMEM((3, features, stick_width), bf16),
            pltpu.VMEM((width + stick_width, features), bf16),
            pltpu.VMEM((4, heads, rows, dm), bf16),
            pltpu.VMEM((4, heads, rows, dm), bf16),
            pltpu.VMEM((4, heads, rows, dm), f32),
            pltpu.VMEM((4, heads, rows, dm), bf16),
            pltpu.VMEM((rows, stick_width), bf16),
            pltpu.VMEM((n_sp, 2, rows, stick_width), bf16),
            pltpu.VMEM((heads, rows, ds), f32),
            pltpu.VMEM((heads, rows, ds), f32),
            pltpu.VMEM((16, features), bf16),
            pltpu.VMEM((lanes, rows), f32),
            pltpu.VMEM((rows, lanes), f32),
            pltpu.VMEM((8, lanes), f32),
            pltpu.VMEM((heads, dm, dm), f32),
            pltpu.VMEM((heads, dm, dm), bf16),
            pltpu.VMEM((heads, dm, dm), bf16),
            pltpu.VMEM((8, lanes), f32),
            pltpu.VMEM((8, lanes), f32),
            pltpu.VMEM((rows, width + stick_width), bf16),
            pltpu.VMEM((n_out, half, features // n_out), bf16),
            pltpu.VMEM((n_out, half, features // n_out), bf16),
            dma((9,)),
            dma((1,)),
            dma((1,)),
            dma((2 * heads,)),
            dma((2 * heads,)),
            dma((2 * heads,)),
            dma((2 * heads,)),
            dma((4 * heads,)),
            dma((4 * heads,)),
            dma((4 * heads,)),
            dma((4 * heads,)),
            dma((n_sp,)),
            dma((n_sp,)),
            dma((2 * heads,)),
            dma((2 * heads,)),
            dma((1,)),
            dma((1,)),
            dma((n_out,)),
            dma((n_out,)),
        ],
        compiler_params=pltpu.CompilerParams(
            collective_id=0, has_side_effects=True, vmem_limit_bytes=60 * 1024 * 1024
        ),
    )(
        tokens[0],
        norm_gain[None],
        memory_ingate.T,
        memory_forget.T,
        forget_bias,
        forget_shift[0].T,
        stick_bias,
        memory_gain[None],
        stick_gain[None],
        memory_key,
        memory_value,
        memory_query,
        memory_outgate,
        stick_query,
        stick_key,
        stick_value,
        out_memory,
        out_stick,
    )
    return out[None]


def solution(mesh):
    assert mesh.shape["fs"] == 4 and mesh.shape["tp"] == 2
    return jax.shard_map(
        functools.partial(per_device, mesh.shape["sp"]),
        mesh=mesh,
        in_specs=(
            P("fs", "sp", "tp"),
            P(),
            P("fs", "tp"),
            P("fs", "tp"),
            P("fs", "tp"),
            P("fs", "tp"),
            P(None, "tp"),
            P(None, "tp"),
            P("tp"),
            P("fs", "sp", "tp"),
            P(None, "tp"),
            P(None, "tp"),
            P(None, "tp"),
            P("tp"),
            P("tp"),
            P("tp"),
            P("tp", None),
            P("tp", None),
        ),
        out_specs=P("fs", ("sp", "tp"), None),
        check_vma=False,
    )
```

```python
import functools

import jax
import jax.numpy as jnp
from jax import lax
from jax.experimental import pallas as pl
from jax.experimental.pallas import tpu as pltpu
from jax.sharding import PartitionSpec as P

MESH = pl.DeviceIdType.MESH
epsilon = 1e-06
floor_neg = -1e30
f32 = jnp.float32
bf16 = jnp.bfloat16

KEY, VALUE, QUERY, GATE = 0, 1, 2, 3


def dot(a, b, dims=((1,), (0,))):
    return lax.dot_general(a, b, (dims, ((), ())), preferred_element_type=f32)


def softplus(z):
    return jnp.maximum(z, 0.0) + jnp.log(1.0 + jnp.exp(-jnp.abs(z)))


def kernel(
    n_sp,
    n_out,
    tok_ref,
    gain_ref,
    ingate_ref,
    forget_ref,
    bias_ref,
    shift_ref,
    sbias_ref,
    mgain_ref,
    sgain_ref,
    wk_hbm,
    wv_hbm,
    wq_hbm,
    wo_hbm,
    sq_hbm,
    sk_hbm,
    sv_hbm,
    om_hbm,
    os_hbm,
    out_ref,
    tok_in,
    nrm,
    xg,
    wm,
    wg,
    ws,
    wout,
    sb,
    rb,
    own_part,
    proj,
    squery,
    kv,
    stick_acc,
    stick_run,
    gw,
    u_rows,
    u_cols,
    totals,
    tops,
    state_own,
    state_in,
    state_out,
    log_in,
    log_out,
    mix,
    ob,
    orb,
    load_sem,
    tok_s,
    tok_r,
    a2a_s,
    a2a_r,
    fwd_s,
    fwd_r,
    w_s,
    w_r,
    rs_s,
    rs_r,
    kv_s,
    kv_r,
    chain_s,
    chain_r,
    log_s,
    log_r,
    out_s,
    out_r,
):
    f = lax.axis_index("fs")
    s = lax.axis_index("sp")
    t = lax.axis_index("tp")
    rows, half_feat = tok_ref.shape
    heads = state_own.shape[0]
    dm = state_own.shape[1]
    ds = sgain_ref.shape[1] // heads
    block = wm.shape[1]
    half = rows // 2
    other = 1 - t

    def flip(bits):
        if bits == 3:
            return 3 - f
        if bits == 1:
            return f + 1 - 2 * (f % 2)
        return f + 2 - 4 * (f // 2)

    def remote(src, dst, send, recv, device):
        return pltpu.make_async_remote_copy(
            src_ref=src,
            dst_ref=dst,
            send_sem=send,
            recv_sem=recv,
            device_id=device,
            device_id_type=MESH,
        )

    barrier = pltpu.get_barrier_semaphore()
    pl.semaphore_signal(barrier, inc=1, device_id={"tp": other}, device_id_type=MESH)
    for bits in (1, 2, 3):
        pl.semaphore_signal(barrier, inc=1, device_id={"fs": flip(bits)}, device_id_type=MESH)

    @pl.when(s > 0)
    def _():
        pl.semaphore_signal(barrier, inc=1, device_id={"sp": s - 1}, device_id_type=MESH)

    @pl.when(s < n_sp - 1)
    def _():
        pl.semaphore_signal(barrier, inc=1, device_id={"sp": s + 1}, device_id_type=MESH)

    width_s = ws.shape[2]
    loads = [
        pltpu.make_async_copy(sq_hbm, ws.at[0], load_sem.at[0]),
        pltpu.make_async_copy(sk_hbm, ws.at[1], load_sem.at[1]),
        pltpu.make_async_copy(sv_hbm, ws.at[2], load_sem.at[2]),
        pltpu.make_async_copy(wk_hbm, wm.at[0], load_sem.at[3]),
        pltpu.make_async_copy(wv_hbm, wm.at[1], load_sem.at[4]),
        pltpu.make_async_copy(wq_hbm, wm.at[2], load_sem.at[5]),
        pltpu.make_async_copy(wo_hbm, wm.at[3], load_sem.at[6]),
        pltpu.make_async_copy(om_hbm, wout.at[pl.ds(0, heads * dm)], load_sem.at[7]),
        pltpu.make_async_copy(os_hbm, wout.at[pl.ds(heads * dm, heads * ds)], load_sem.at[8]),
    ]
    for at in (3, 4, 0, 1, 2, 5, 6, 7, 8):
        loads[at].start()

    peers = 4 + jnp.where(s > 0, 1, 0) + jnp.where(s < n_sp - 1, 1, 0)
    pl.semaphore_wait(barrier, peers)

    tok_copy = remote(tok_ref, tok_in, tok_s.at[0], tok_r.at[0], {"tp": other})
    tok_copy.start()

    def pair_bits(h):
        return 1 if h % 2 == 0 else 2

    def sum_bits(h):
        return 3 - pair_bits(h)

    def weight_copy(p, h):
        at = p * heads + h
        return remote(
            wm.at[p, :, pl.ds(h * dm, dm)], wg.at[p, h], w_s.at[at], w_r.at[at],
            {"fs": flip(pair_bits(h))},
        )

    def send_weight(p):
        loads[3 + p].wait()
        for h in range(heads):
            weight_copy(p, h).start()

    send_weight(KEY)
    tok_copy.wait_recv()

    step_rows = 32
    own_cols = pl.ds(pl.multiple_of(t * half_feat, half_feat), half_feat)
    far_cols = pl.ds(pl.multiple_of(other * half_feat, half_feat), half_feat)

    def norm_rows(i, _):
        at = pl.ds(pl.multiple_of(i * step_rows, step_rows), step_rows)
        own = tok_ref[at, :].astype(f32)
        far = tok_in[at, :].astype(f32)
        total = jnp.sum(own * own, axis=1, keepdims=True) + jnp.sum(far * far, axis=1, keepdims=True)
        scale = lax.rsqrt(total / (2 * half_feat) + epsilon)
        nrm[at, own_cols] = (own * scale * gain_ref[:, own_cols]).astype(bf16)
        nrm[at, far_cols] = (far * scale * gain_ref[:, far_cols]).astype(bf16)
        return 0

    lax.fori_loop(0, rows // step_rows, norm_rows, 0)

    my_rows = pl.ds(pl.multiple_of(t * half, half), half)

    def feature_block(index):
        return pl.ds(pl.multiple_of(index * block, block), block)

    a2a, fwd = {}, {}
    for h in range(heads):
        for which in range(2):
            at = h * 2 + which
            to = flip(sum_bits(h))
            a2a[at] = remote(
                nrm.at[my_rows, feature_block(to if which == 0 else flip(3))],
                xg.at[h, which, my_rows],
                a2a_s.at[at],
                a2a_r.at[at],
                {"fs": to},
            )
            a2a[at].start()
    send_weight(VALUE)

    for load in loads[:3]:
        load.wait()
    normed = nrm[...]
    kv[0, 0] = dot(normed, ws[1]).astype(bf16)
    kv[0, 1] = dot(normed, ws[2]).astype(bf16)

    def kv_copy(d):
        return remote(kv.at[d - 1], kv.at[d], kv_s.at[d], kv_r.at[d], {"sp": s + 1})

    def kv_send(d):
        @pl.when((s < n_sp - 1) & (s >= d - 1))
        def _():
            kv_copy(d).start()

    kv_send(1)
    squery[...] = dot(normed, ws[0]).astype(bf16)

    row_at = lax.broadcasted_iota(jnp.int32, (rows, rows), 0)
    col_at = lax.broadcasted_iota(jnp.int32, (rows, rows), 1)
    gw[...] = jnp.zeros(gw.shape, bf16)
    gw[0:heads, :] = ingate_ref[...]
    gw[8 : 8 + heads, :] = forget_ref[...]
    gate = dot(gw[...], normed, ((1,), (1,)))
    triu = (row_at <= col_at).astype(f32)
    u_rows[...] = jnp.zeros(u_rows.shape, f32)
    for h in range(heads):
        log_forget = shift_ref[h : h + 1, :] - softplus(-(gate[8 + h : 9 + h, :] + bias_ref[h]))
        cumulative = lax.dot_general(
            jnp.broadcast_to(log_forget, (8, rows)), triu, (((1,), (0,)), ((), ())),
            precision=lax.Precision.HIGHEST, preferred_element_type=f32,
        )
        u_rows[h : h + 1, :] = gate[h : h + 1, :] - cumulative[0:1, :]
        totals[h : h + 1, :] = jnp.broadcast_to(
            cumulative[0:1, rows - 1 : rows], (1, totals.shape[1])
        )
    u_cols[...] = jnp.transpose(u_rows[...])

    def stick_part(h, kv_at, diagonal):
        cols = slice(h * ds, (h + 1) * ds)
        z = dot(squery[:, cols], kv[kv_at, 0, :, cols], ((1,), (1,)))
        z = z * ds ** (-0.5) + sbias_ref[h]
        keep = -softplus(z)
        visible = col_at < row_at
        if diagonal:
            kept = jnp.where(visible, keep, 0.0)
        else:
            kept = keep
        strict = (row_at > col_at).astype(bf16)
        high = kept.astype(bf16)
        low = (kept - high.astype(f32)).astype(bf16)
        after = dot(high, strict) + dot(low, strict)
        weights = jnp.exp(z + keep + after)
        if diagonal:
            weights = jnp.where(visible, weights, 0.0)
        part = dot(weights.astype(bf16), kv[kv_at, 1, :, cols])
        return part, jnp.sum(kept, axis=1, keepdims=True)

    def stick_own():
        for h in range(heads):
            part, keep = stick_part(h, 0, True)
            stick_acc[h] = part
            stick_run[h] = jnp.broadcast_to(keep, stick_run.shape[1:])

    def stick_span(d):
        @pl.when(s >= d)
        def _():
            remote(kv.at[d - 1], kv.at[d], kv_s.at[d], kv_r.at[d], {"sp": s - 1}).wait_recv()

        kv_next(d)

        @pl.when(s >= d)
        def _():
            for h in range(heads):
                part, keep = stick_part(h, d, False)
                stick_acc[h] = stick_acc[h] + jnp.exp(stick_run[h]) * part
                stick_run[h] = stick_run[h] + keep

    def kv_next(d):
        @pl.when((s < n_sp - 1) & (s >= d) & (d < n_sp - 1))
        def _():
            kv_copy(d + 1).start()

    def stick_spans(low, high):
        if high > low:
            lax.fori_loop(low, high, lambda d, c: (stick_span(d), c)[1], 0)

    stick_own()
    for at in range(2 * heads):
        a2a[at].wait_recv()
        h, which = divmod(at, 2)
        fwd[at] = remote(
            xg.at[h, which, my_rows],
            xg.at[h, which, my_rows],
            fwd_s.at[at],
            fwd_r.at[at],
            {"tp": other},
        )
        fwd[at].start()

    def rs_copy(p, h):
        at = p * heads + h
        return remote(
            sb.at[p, h], rb.at[p, h], rs_s.at[at], rs_r.at[at], {"fs": flip(sum_bits(h))}
        )

    def partials(p):
        for h in range(heads):
            cols = slice(h * dm, (h + 1) * dm)
            if p == KEY:
                fwd[2 * h].wait_recv()
                fwd[2 * h + 1].wait_recv()
            weight_copy(p, h).wait_recv()
            sb[p, h] = (dot(xg[h, 0], wm[p, :, cols]) + dot(xg[h, 1], wg[p, h])).astype(bf16)
            rs_copy(p, h).start()

    def own_partials(p):
        for h in range(heads):
            cols = slice(h * dm, (h + 1) * dm)
            own_part[p, h] = dot(nrm[:, feature_block(f)], wm[p, :, cols]) + dot(
                nrm[:, feature_block(flip(pair_bits(h)))], wg[p, h]
            )

    def finish(p, h):
        rs_copy(p, h).wait_recv()
        return (own_part[p, h] + rb[p, h].astype(f32)).astype(bf16)

    partials(KEY)
    own_partials(KEY)
    partials(VALUE)
    send_weight(QUERY)
    send_weight(GATE)
    own_partials(VALUE)
    stick_spans(1, min(2, n_sp))

    def column(h):
        return u_cols[:, h : h + 1]

    for h in range(heads):
        proj[KEY, h] = (finish(KEY, h).astype(f32) * dm ** (-0.5)).astype(bf16)
        proj[VALUE, h] = finish(VALUE, h)
        u = column(h)
        top = jnp.max(u, axis=0, keepdims=True)
        weighted = (proj[KEY, h].astype(f32) * jnp.exp(u - top)).astype(bf16)
        state_own[h] = dot(weighted, proj[VALUE, h], ((0,), (0,)))

    def log_copy(to):
        return remote(log_out, log_in, log_s.at[0], log_r.at[0], {"sp": to})

    piece_dm = dm // 2
    pieces = 4

    def chain_copy(h, c, to):
        lines = pl.ds(c // 2 * piece_dm, piece_dm)
        cols = pl.ds(c % 2 * piece_dm, piece_dm)
        at = h * pieces + c
        return remote(
            state_out.at[h, lines, cols], state_in.at[h, lines, cols], chain_s.at[at], chain_r.at[at],
            {"sp": to},
        )

    def chain():
        @pl.when(s == 0)
        def _():
            log_in[...] = jnp.full(log_in.shape, floor_neg, f32)
            state_in[...] = jnp.zeros(state_in.shape, bf16)

        @pl.when(s > 0)
        def _():
            log_copy(s - 1).wait_recv()

        factors = []
        for h in range(heads):
            total = totals[h : h + 1, 0:1]
            early = total + log_in[h : h + 1, 0:1]
            late = total + jnp.max(column(h), axis=0, keepdims=True)
            top = jnp.maximum(early, late)
            log_out[h : h + 1, :] = jnp.broadcast_to(top, (1, log_out.shape[1]))
            factors.append((jnp.exp(early - top), jnp.exp(late - top)))

        @pl.when(s < n_sp - 1)
        def _():
            log_copy(s + 1).start()

        for at in range(pieces * heads):
            h, c = divmod(at, pieces)
            lines = pl.ds(c // 2 * piece_dm, piece_dm)
            cols = pl.ds(c % 2 * piece_dm, piece_dm)

            @pl.when(s > 0)
            def _():
                chain_copy(h, c, s - 1).wait_recv()

            @pl.when(s < n_sp - 1)
            def _():
                early, late = factors[h]
                state_out[h, lines, cols] = (
                    early * state_in[h, lines, cols].astype(f32) + late * state_own[h, lines, cols]
                ).astype(bf16)
                chain_copy(h, c, s + 1).start()

    log_out[...] = jnp.zeros(log_out.shape, f32)
    pl.when(s == 0)(chain)
    stick_spans(2, min(3, n_sp))
    partials(QUERY)
    pl.when(s == 1)(chain)
    own_partials(QUERY)
    pl.when(s == 2)(chain)
    partials(GATE)
    own_partials(GATE)
    stick_spans(3, n_sp)
    for load in loads[7:]:
        load.wait()

    for h in range(heads):
        cols = slice(h * ds, (h + 1) * ds)
        out = stick_acc[h]
        scale = lax.rsqrt(jnp.mean(out * out, axis=1, keepdims=True) + epsilon)
        mix[:, heads * dm + h * ds : heads * dm + (h + 1) * ds] = (
            out * scale * sgain_ref[:, cols]
        ).astype(bf16)

    causal = col_at <= row_at
    for h in range(heads):
        proj[QUERY, h] = finish(QUERY, h)
        masked = jnp.where(causal, u_rows[h : h + 1, :], floor_neg)
        top = jnp.max(masked, axis=1, keepdims=True)
        scores = dot(proj[QUERY, h], proj[KEY, h], ((1,), (1,))) * jnp.exp(masked - top)
        own_part[QUERY, h] = dot(scores.astype(bf16), proj[VALUE, h])
        tops[h] = jnp.broadcast_to(top, tops.shape[1:])
    pl.when(s > 2)(chain)
    for h in range(heads):
        carried_max = log_in[h : h + 1, 0:1]
        top = tops[h, :, 0:1]
        running = jnp.maximum(carried_max, top)
        own_part[QUERY, h] = jnp.exp(top - running) * own_part[QUERY, h] + jnp.exp(
            carried_max - running
        ) * dot(proj[QUERY, h], state_in[h])
    for h in range(heads):
        gated = own_part[QUERY, h] / (1.0 + jnp.exp(-finish(GATE, h).astype(f32)))
        scale = lax.rsqrt(jnp.mean(gated * gated, axis=1, keepdims=True) + epsilon)
        cols = slice(h * dm, (h + 1) * dm)
        mix[:, cols] = (gated * scale * mgain_ref[:, cols]).astype(bf16)

    piece = wout.shape[1] // n_out
    far_rows = pl.ds(pl.multiple_of(other * half, half), half)
    copies = []
    for c in range(n_out):
        cols = slice(c * piece, (c + 1) * piece)
        ob[c] = dot(mix[far_rows, :], wout[:, cols]).astype(bf16)
        copy = remote(ob.at[c], orb.at[c], out_s.at[c], out_r.at[c], {"tp": other})
        copy.start()
        copies.append(copy)
    for c in range(n_out):
        cols = slice(c * piece, (c + 1) * piece)
        mine = dot(mix[my_rows, :], wout[:, cols])
        copies[c].wait_recv()
        out_ref[:, cols] = (mine + orb[c].astype(f32)).astype(bf16)

    tok_copy.wait_send()
    for at in range(2 * heads):
        a2a[at].wait_send()
        fwd[at].wait_send()
    for p in range(4):
        for h in range(heads):
            weight_copy(p, h).wait_send()
            rs_copy(p, h).wait_send()
    for copy in copies:
        copy.wait_send()

    @pl.when(s < n_sp - 1)
    def _():
        log_copy(s + 1).wait_send()
        for at in range(pieces * heads):
            chain_copy(at // pieces, at % pieces, s + 1).wait_send()

    def kv_done(d, c):
        @pl.when((s < n_sp - 1) & (s >= d - 1))
        def _():
            kv_copy(d).wait_send()

        return c

    if n_sp > 1:
        lax.fori_loop(1, n_sp, kv_done, 0)


def per_device(
    n_sp,
    tokens,
    norm_gain,
    memory_query,
    memory_key,
    memory_value,
    memory_outgate,
    memory_ingate,
    memory_forget,
    forget_bias,
    forget_shift,
    stick_query,
    stick_key,
    stick_value,
    stick_bias,
    memory_gain,
    stick_gain,
    out_memory,
    out_stick,
):
    rows, half_feat = tokens.shape[1:]
    features = 2 * half_feat
    heads = forget_bias.shape[0]
    block, width = memory_query.shape
    dm = width // heads
    stick_width = stick_query.shape[1]
    ds = stick_width // heads
    lanes = 128
    n_out = 4
    half = rows // 2

    vmem = pl.BlockSpec(memory_space=pltpu.VMEM)
    smem = pl.BlockSpec(memory_space=pltpu.SMEM)
    anyw = pl.BlockSpec(memory_space=pl.ANY)
    dma = pltpu.SemaphoreType.DMA
    out = pl.pallas_call(
        functools.partial(kernel, n_sp, n_out),
        out_shape=pltpu.VMEM((half, features), bf16),
        in_specs=[vmem] * 4 + [smem, vmem, smem] + [vmem] * 2 + [anyw] * 9,
        out_specs=vmem,
        scratch_shapes=[
            pltpu.VMEM((rows, half_feat), bf16),
            pltpu.VMEM((rows, features), bf16),
            pltpu.VMEM((heads, 2, rows, block), bf16),
            pltpu.VMEM((4, block, width), bf16),
            pltpu.VMEM((4, heads, block, dm), bf16),
            pltpu.VMEM((3, features, stick_width), bf16),
            pltpu.VMEM((width + stick_width, features), bf16),
            pltpu.VMEM((4, heads, rows, dm), bf16),
            pltpu.VMEM((4, heads, rows, dm), bf16),
            pltpu.VMEM((4, heads, rows, dm), f32),
            pltpu.VMEM((4, heads, rows, dm), bf16),
            pltpu.VMEM((rows, stick_width), bf16),
            pltpu.VMEM((n_sp, 2, rows, stick_width), bf16),
            pltpu.VMEM((heads, rows, ds), f32),
            pltpu.VMEM((heads, rows, ds), f32),
            pltpu.VMEM((16, features), bf16),
            pltpu.VMEM((lanes, rows), f32),
            pltpu.VMEM((rows, lanes), f32),
            pltpu.VMEM((8, lanes), f32),
            pltpu.VMEM((heads, rows, lanes), f32),
            pltpu.VMEM((heads, dm, dm), f32),
            pltpu.VMEM((heads, dm, dm), bf16),
            pltpu.VMEM((heads, dm, dm), bf16),
            pltpu.VMEM((8, lanes), f32),
            pltpu.VMEM((8, lanes), f32),
            pltpu.VMEM((rows, width + stick_width), bf16),
            pltpu.VMEM((n_out, half, features // n_out), bf16),
            pltpu.VMEM((n_out, half, features // n_out), bf16),
            dma((9,)),
            dma((1,)),
            dma((1,)),
            dma((2 * heads,)),
            dma((2 * heads,)),
            dma((2 * heads,)),
            dma((2 * heads,)),
            dma((4 * heads,)),
            dma((4 * heads,)),
            dma((4 * heads,)),
            dma((4 * heads,)),
            dma((n_sp,)),
            dma((n_sp,)),
            dma((4 * heads,)),
            dma((4 * heads,)),
            dma((1,)),
            dma((1,)),
            dma((n_out,)),
            dma((n_out,)),
        ],
        compiler_params=pltpu.CompilerParams(
            collective_id=0, has_side_effects=True, vmem_limit_bytes=60 * 1024 * 1024
        ),
    )(
        tokens[0],
        norm_gain[None],
        memory_ingate.T,
        memory_forget.T,
        forget_bias,
        forget_shift[0].T,
        stick_bias,
        memory_gain[None],
        stick_gain[None],
        memory_key,
        memory_value,
        memory_query,
        memory_outgate,
        stick_query,
        stick_key,
        stick_value,
        out_memory,
        out_stick,
    )
    return out[None]


def solution(mesh):
    assert mesh.shape["fs"] == 4 and mesh.shape["tp"] == 2
    return jax.shard_map(
        functools.partial(per_device, mesh.shape["sp"]),
        mesh=mesh,
        in_specs=(
            P("fs", "sp", "tp"),
            P(),
            P("fs", "tp"),
            P("fs", "tp"),
            P("fs", "tp"),
            P("fs", "tp"),
            P(None, "tp"),
            P(None, "tp"),
            P("tp"),
            P("fs", "sp", "tp"),
            P(None, "tp"),
            P(None, "tp"),
            P(None, "tp"),
            P("tp"),
            P("tp"),
            P("tp"),
            P("tp", None),
            P("tp", None),
        ),
        out_specs=P("fs", ("sp", "tp"), None),
        check_vma=False,
    )
```
